32 devices in a mesh: ep: 4 (over y, x), tp: 8 (over z, core).
Axes of the slice: x: 2, y: 2, z: 4, core: 2. Of those that a mesh axis runs over, the one named last changes fastest.
Arguments:
- tokens: bfloat16 [128, 4096], P('ep', 'tp'), may hold values from -16 to 16
- routing: int32 [128, 4], P('ep'), may hold values from 0 to 7, all different within a row; in each aligned block of 32 rows (0 to 31, 32 to 63, ...) at most 32 rows name the same one
- gate_weights: float32 [128, 4], P('ep'), may hold values from 0.1 to 1
- w_gate: bfloat16 [8, 1024, 4096], P('ep', 'tp'), may hold values from -0.09375 to 0.09375
- w_up: bfloat16 [8, 1024, 4096], P('ep', 'tp'), may hold values from -0.09375 to 0.09375
- w_down: bfloat16 [8, 1024, 4096], P('ep', None, 'tp'), may hold values from -2 to 2
- out_gain: float32 [4096], P('tp'), may hold values from 0.1 to 1.9
Outputs:
- mixed: bfloat16 [128, 4096], P('ep', 'tp')
The draws below stay inside these ranges and needn't reach their ends.
Inputs may be any that keep to these rules, and one draw needn't show every extreme that they name: `routing`: in each aligned block of 32 rows (the tokens of one index of ep) no expert is named by more than 32 entries, and in every draw some expert is named by exactly 32 entries of some block. The 4 entries of a row differ.
All inputs are finite; a program needn't handle non-finite values.
Results may differ from the reference program's by a relative error of at most 0.0057.
Values may be sent and summed in bfloat16 or wider, within the bound.
A program may use at most 64 MiB of HBM per device.

```python
import math
import jax
import jax.numpy as jnp
import numpy as np
from jax import lax

D = 4096
FE = 1024
TOPK = 4
EXP_DEV = 2
EXPERTS = 8
TOK_EP = 32
TOKENS = 128
CAP = 32
N_EP = 4


def draw_tokens(key, part):
    first_key, second_key = jax.random.split(key)
    base = jnp.clip(jax.random.normal(first_key, (TOKENS, D), jnp.float32), -4.5, 4.5)
    row_factor = jnp.exp(jax.random.uniform(second_key, (TOKENS, 1), jnp.float32, -1.2, 1.2))
    return (base * row_factor).astype(jnp.bfloat16)


def draw_w_down(key, part):
    first_key, second_key = jax.random.split(jax.random.fold_in(key, 7))
    base = jnp.clip(jax.random.normal(first_key, (EXPERTS, FE, D), jnp.float32), -4.5, 4.5) * FE ** (-0.5)
    group_factor = jnp.exp(jax.random.uniform(second_key, (16,), jnp.float32, -1.1, 1.1))
    column_factor = jnp.repeat(group_factor, D // 16)
    return (base * column_factor[None, None, :]).astype(jnp.bfloat16)


def block_levels(rng, shape, shards, low, largest):
    loudness = 1.0
    for position, parts in shards:
        heights = jax.random.uniform(jax.random.fold_in(jax.random.fold_in(rng, 6), position), (parts,), jnp.float32, low / len(shards), largest / len(shards))
        loudness = loudness * jnp.repeat(jnp.exp(heights), shape[position] // parts).reshape((-1,) + (1,) * (len(shape) - 1 - position))
    return loudness


def deal_out(own_key, own, number, rows, number_of, top, bound, lean):
    order = jax.random.permutation(own_key, number_of)
    packed, usual = portions_of(number_of, rows * top, bound, lean, True), portions_of(number_of, rows * top, bound, lean, False)
    places = jnp.arange(number_of)

    def named(tallies, offset_by):
        used = int((tallies > 0).sum())
        fixed = max(1, used // 4)
        moved = fixed + (places - fixed + offset_by * (used - fixed)) % max(1, number_of - fixed)
        return jnp.zeros((number_of,), jnp.int32).at[order[jnp.where(places < fixed, places, moved)]].set(jnp.asarray(tallies, jnp.int32))

    tallies = jnp.where(number % 4 == 0, named(packed, number // 4), named(usual, number - number // 4 - 1))
    mixed = jax.random.permutation(jax.random.fold_in(own, 3), number_of)
    giver, receiver = mixed[0:number_of // 2 * 2:2], mixed[1:number_of // 2 * 2:2]
    slack = jnp.minimum(tallies[giver] - 1, bound - tallies[receiver]) // 2
    slack = jnp.where((giver == order[0]) | (receiver == order[0]) | (tallies[receiver] == 0), 0, jnp.maximum(slack, 0))
    moved = jax.random.randint(jax.random.fold_in(own, 4), (number_of // 2,), 0, 1 << 20) % (slack + 1)
    tallies = tallies.at[giver].add(-moved).at[receiver].add(moved)
    labels = jnp.searchsorted(jnp.cumsum(tallies), jnp.arange(rows * top), side="right").astype(jnp.int32)
    grid = labels.reshape(top, rows).T
    grid = grid[jax.random.permutation(jax.random.fold_in(own, 1), rows)]
    offset_by = jax.random.randint(jax.random.fold_in(own, 2), (rows, 1), 0, top)
    return jnp.take_along_axis(grid, (jnp.arange(top)[None, :] + offset_by) % top, axis=1)


def portions_of(number_of, total, bound, skew, full):
    portions = [(1 << 20) // math.isqrt(grade ** skew) + 1 for grade in range(1, number_of + 1)]
    largest = bound if full else min(bound, max(-(-total // number_of), total * portions[0] // sum(portions)))
    least = 1 if total - largest >= number_of - 1 else 0
    given, spare = [largest] + [least] * (number_of - 1), total - largest - least * (number_of - 1)
    while spare > 0:
        candidates = [i for i in range(1, number_of) if given[i] < largest] or [i for i in range(1, number_of) if given[i] < bound]
        whole, budget = sum([portions[i] for i in candidates]), spare
        for i in candidates:
            extra = min(bound - given[i], max(1, budget * portions[i] // whole), spare)
            given[i] = given[i] + extra
            spare = spare - extra
    return np.array(given)


def scatter_about(own_key, extent, scale, reach, cuts=(), kind=jnp.bfloat16):
    factor_of = block_levels(own_key, extent, cuts, -0.22, 0.18) if cuts else 1.0
    drawn = jax.random.normal(own_key, extent, jnp.float32) * scale * factor_of
    return jnp.minimum(jnp.maximum(drawn, -reach), reach).astype(kind)


def setup_inputs(seed: int = 0) -> dict:
    key_of = jax.random.split(jax.random.key(seed), 8)
    tokens = draw_tokens(jax.random.fold_in(key_of[7], 71), 0)
    routing_keys = jax.random.split(jax.random.fold_in(key_of[1], 1), TOKENS // TOK_EP)
    routing_turns = jax.random.permutation(jax.random.fold_in(key_of[1], 3), TOKENS // TOK_EP)
    routing = jax.vmap(lambda own, number: deal_out(jax.random.fold_in(key_of[1], 2), own, number, TOK_EP, EXPERTS, TOPK, CAP, 2))(routing_keys, routing_turns).reshape((TOKENS, TOPK))
    gate_weights = jnp.clip(0.1 + 0.9 * jax.random.uniform(key_of[2], (TOKENS, TOPK), jnp.float32) ** block_levels(key_of[2], (TOKENS, TOPK), ((0, 4),), -0.2, 0.2), 0.1, 1.0)
    w_gate = scatter_about(key_of[3], (EXPERTS, FE, D), D ** -0.5, 0.09375, ((0, 4), (1, 8)))
    w_up = scatter_about(key_of[4], (EXPERTS, FE, D), D ** -0.5, 0.09375, ((0, 4), (1, 8)))
    w_down = draw_w_down(jax.random.fold_in(key_of[7], 71), 0)
    out_gain = jnp.clip(1.0 + 0.18 * jax.random.normal(key_of[6], (D,), jnp.float32), 0.1, 1.9)
    return {"tokens": tokens, "routing": routing, "gate_weights": gate_weights, "w_gate": w_gate, "w_up": w_up, "w_down": w_down, "out_gain": out_gain}


norm_eps = 1e-05

def reference(tokens, routing, gate_weights, w_gate, w_up, w_down, out_gain):
    experts = EXP_DEV * N_EP
    rows_max = N_EP * CAP
    token_f = tokens.astype(jnp.float32)
    row_scale = lax.rsqrt(lax.optimization_barrier(jnp.mean(token_f * token_f, axis=1)) + norm_eps)
    flat_route = routing.reshape(-1).astype(jnp.int32)
    entry_count = flat_route.shape[0]
    expert_ids = jnp.arange(experts, dtype=jnp.int32)
    hit_table = (flat_route[:, None] == expert_ids[None, :]).astype(jnp.int32)
    running = jnp.cumsum(hit_table, axis=0).astype(jnp.int32) - hit_table
    slot_rank = lax.optimization_barrier(jnp.sum(running * hit_table, axis=1)).astype(jnp.int32)
    owner = (jnp.arange(entry_count, dtype=jnp.int32) // TOPK).astype(jnp.int32)

    def one_expert(inputs):
        expert_id, gate_mat, up_mat, down_mat = inputs
        target = jnp.where(flat_route == expert_id, slot_rank, rows_max).astype(jnp.int32)
        row_ids = jnp.zeros((rows_max,), jnp.int32).at[target].set(owner, mode='drop')
        picked_rows = tokens[row_ids]
        scale_rows = row_scale[row_ids][:, None]
        gate_pre = jnp.dot(picked_rows, gate_mat.T, preferred_element_type=jnp.float32) * scale_rows
        up_pre = jnp.dot(picked_rows, up_mat.T, preferred_element_type=jnp.float32) * scale_rows
        hidden = (jax.nn.silu(gate_pre) * up_pre).astype(jnp.bfloat16)
        return jnp.dot(hidden, down_mat, preferred_element_type=jnp.float32).astype(jnp.bfloat16)
    expert_outs = lax.map(one_expert, (expert_ids, w_gate, w_up, w_down))
    chosen = expert_outs[flat_route, slot_rank].astype(jnp.float32).reshape(TOKENS, TOPK, D)
    combined = lax.optimization_barrier(jnp.sum(chosen * gate_weights[:, :, None], axis=1))
    final_scale = lax.rsqrt(lax.optimization_barrier(jnp.mean(combined * combined, axis=1)) + norm_eps)
    return (combined * final_scale[:, None] * out_gain[None, :]).astype(jnp.bfloat16)
```

```python
import functools

import jax
import jax.numpy as jnp
from jax import lax
from jax.experimental import pallas as pl
from jax.experimental.pallas import tpu as pltpu
from jax.sharding import PartitionSpec as P

D = 4096
TOPK = 4
EXP_DEV = 2


norm_eps = 1e-05


def routed_body(tokens, routing, gate_weights, w_gate, w_up, w_down, out_gain):
    ep_count = lax.axis_size("ep")
    tok_rows = tokens.shape[0]
    width_part = tokens.shape[1]
    experts = EXP_DEV * ep_count
    slot_count = 2 * tok_rows * TOPK // experts
    span_rows = ep_count * slot_count
    total_slots = EXP_DEV * span_rows
    flat_route = routing.reshape(-1)
    expert_ids = jnp.arange(experts, dtype=jnp.int32)
    hit_table = (flat_route[:, None] == expert_ids[None, :]).astype(jnp.int32)
    running = jnp.cumsum(hit_table, axis=0) - hit_table
    slot_rank = jnp.sum(running * hit_table, axis=1)
    slot_target = flat_route % EXP_DEV * span_rows + flat_route // EXP_DEV * slot_count + slot_rank
    entry_targets = slot_target.reshape(tok_rows, TOPK)
    slot_ids = jnp.arange(total_slots, dtype=jnp.int32)
    select_table = jnp.any(entry_targets[None, :, :] == slot_ids[:, None, None], axis=2).astype(
        jnp.bfloat16
    )
    outgoing = jnp.dot(select_table, tokens, preferred_element_type=jnp.float32).astype(
        jnp.bfloat16
    )
    outgoing = outgoing.reshape(EXP_DEV, ep_count, slot_count, width_part)
    arrived = lax.all_to_all(outgoing, "ep", split_axis=1, concat_axis=1, tiled=True).reshape(
        EXP_DEV, span_rows, width_part
    )
    piece_cols = lax.all_gather(arrived, "tp", axis=2, tiled=True)
    gate_sum = jnp.einsum("efn,esn->efs", w_gate, piece_cols, preferred_element_type=jnp.float32)
    up_sum = jnp.einsum("efn,esn->efs", w_up, piece_cols, preferred_element_type=jnp.float32)
    square_sum = jnp.einsum(
        "esn,esn->es", piece_cols, piece_cols, preferred_element_type=jnp.float32
    )
    row_scale = lax.rsqrt(square_sum / D + norm_eps)[:, None, :]
    hidden = (jax.nn.silu(gate_sum * row_scale) * (up_sum * row_scale)).astype(jnp.bfloat16)
    out_part = w_down.shape[2]
    expert_out = jnp.einsum(
        "ens,end->esd",
        lax.all_gather(hidden, "tp", axis=1, tiled=True),
        w_down,
        preferred_element_type=jnp.float32,
    ).astype(jnp.bfloat16)
    returned = lax.all_to_all(
        expert_out.reshape(EXP_DEV, ep_count, slot_count, out_part),
        "ep",
        split_axis=1,
        concat_axis=1,
        tiled=True,
    )
    returned = returned.reshape(total_slots, out_part)
    chosen = returned[slot_target].astype(jnp.float32).reshape(tok_rows, TOPK, out_part)
    combined = jnp.sum(chosen * gate_weights[:, :, None], axis=1)
    square_total = lax.psum(jnp.sum(combined * combined, axis=1), "tp")
    final_scale = lax.rsqrt(square_total / D + norm_eps)
    return (combined * final_scale[:, None] * out_gain[None, :]).astype(jnp.bfloat16)


MESH = pl.DeviceIdType.MESH
CORES = 2
LANES = 128


def dense_kernel(
    n_ep,
    n_tp,
    tok_hbm,
    route_ref,
    gates_ref,
    wg_hbm,
    wu_hbm,
    wd_hbm,
    gain_ref,
    out_ref,
    x_all,
    g_all,
    w_v,
    wd_v,
    acc,
    h_all,
    p_send,
    p_recv,
    s_send,
    s_all,
    loc_sem,
    snd_sem,
    x_sem,
    g_sem,
    h_sem,
    p_sem,
    s_sem,
):
    e = lax.axis_index("ep")
    t = lax.axis_index("tp")
    n_z = n_tp // CORES
    z = t // CORES
    c = t % CORES
    mate = z * CORES + (1 - c)
    rows, width = tok_hbm.shape
    tokens = rows * n_ep
    n_exp, hid = wg_hbm.shape[0], wg_hbm.shape[1]
    features = wg_hbm.shape[2]
    mine = pl.ds(pl.multiple_of(e * rows, rows), rows)

    barrier = pltpu.get_barrier_semaphore()
    tp_peers = [lax.rem(t + d, n_tp) for d in range(1, n_tp)]
    ep_peers = [lax.rem(e + d, n_ep) for d in range(1, n_ep)]
    z_order = [0]
    for d in range(1, n_z // 2 + 1):
        z_order += [d] if 2 * d == n_z else [d, n_z - d]
    z_list = [lax.rem(z + d, n_z) for d in z_order]
    for peer in tp_peers:
        pl.semaphore_signal(barrier, inc=1, device_id=(e, peer), device_id_type=MESH)
    for peer in ep_peers:
        pl.semaphore_signal(barrier, inc=1, device_id=(peer, t), device_id_type=MESH)

    tok_copy = pltpu.make_async_copy(tok_hbm, x_all.at[t, mine, :], loc_sem.at[0])
    tok_copy.start()
    wg_copy = pltpu.make_async_copy(wg_hbm, w_v.at[0:n_exp], loc_sem.at[1])
    wg_copy.start()
    wu_copy = pltpu.make_async_copy(wu_hbm, w_v.at[n_exp : 2 * n_exp], loc_sem.at[2])
    wu_copy.start()
    wd_copy = pltpu.make_async_copy(wd_hbm, wd_v, loc_sem.at[3])
    wd_copy.start()

    lane = lax.broadcasted_iota(jnp.int32, (rows, LANES), 1)
    table = jnp.zeros((rows, LANES), jnp.float32)
    for k in range(route_ref.shape[1]):
        table += jnp.where(route_ref[:, k : k + 1] == lane, gates_ref[:, k : k + 1], 0.0)
    g_all[mine, :] = table

    sends = []

    def send(src, dst, recv, device):
        copy = pltpu.make_async_remote_copy(
            src_ref=src,
            dst_ref=dst,
            send_sem=snd_sem.at[len(sends)],
            recv_sem=recv,
            device_id=device,
            device_id_type=MESH,
        )
        copy.start()
        sends.append(copy)

    def arrive(dst, recv):
        pltpu.make_async_remote_copy(
            src_ref=dst,
            dst_ref=dst,
            send_sem=snd_sem.at[0],
            recv_sem=recv,
            device_id=(e, mate),
            device_id_type=MESH,
        ).wait_recv()

    def x_block(ep, tp):
        return x_all.at[tp, pl.ds(pl.multiple_of(ep * rows, rows), rows), :]

    def send_x(ep, tp, device):
        send(x_block(ep, tp), x_block(ep, tp), x_sem.at[ep, tp], device)

    tok_copy.wait()
    pl.semaphore_wait(barrier, n_tp - 1 + n_ep - 1)

    for zz in z_list[1:]:
        send_x(e, t, (e, zz * CORES + c))
    for peer in ep_peers:
        send_x(e, t, (peer, t))
    send_x(e, t, (e, mate))
    for peer in ep_peers:
        send(g_all.at[mine, :], g_all.at[mine, :], g_sem.at[e], (peer, t))
    for zz in z_list[1:]:
        tp = zz * CORES + c
        arrive(x_block(e, tp), x_sem.at[e, tp])
        for peer in ep_peers:
            send_x(e, tp, (peer, t))
        send_x(e, tp, (e, mate))
    wg_copy.wait()
    wu_copy.wait()

    square = jnp.zeros((tokens, LANES), jnp.float32)

    def up_part(tp, first, square):
        x = x_all[tp]
        cols = pl.ds(pl.multiple_of(tp * width, width), width)
        w = w_v[:, :, cols].reshape(2 * n_exp * hid, width)
        part = lax.dot_general(
            x, w, (((1,), (1,)), ((), ())), preferred_element_type=jnp.float32
        )
        if first:
            acc[...] = part
        else:
            acc[...] += part
        for i in range(width // LANES):
            piece = x[:, i * LANES : (i + 1) * LANES].astype(jnp.float32)
            square = square + piece * piece
        return square

    for i, zz in enumerate(z_list):
        tp = zz * CORES + c
        for peer in ep_peers:
            arrive(x_block(peer, tp), x_sem.at[peer, tp])
            send_x(peer, tp, (e, mate))
        square = up_part(tp, i == 0, square)
    for zz in z_list:
        tp = zz * CORES + 1 - c
        for ep in [e] + ep_peers:
            arrive(x_block(ep, tp), x_sem.at[ep, tp])
        square = up_part(tp, False, square)
    for peer in ep_peers:
        theirs = g_all.at[pl.ds(pl.multiple_of(peer * rows, rows), rows), :]
        arrive(theirs, g_sem.at[peer])

    scale = lax.rsqrt(jnp.sum(square, axis=1, keepdims=True) / features + norm_eps)
    every_lane = lax.broadcasted_iota(jnp.int32, (tokens, LANES), 1)
    for j in range(n_exp):
        gate = acc[:, j * hid : (j + 1) * hid] * scale
        up = acc[:, (n_exp + j) * hid : (n_exp + j + 1) * hid] * scale
        weight = jnp.sum(
            jnp.where(every_lane == e * n_exp + j, g_all[...], 0.0), axis=1, keepdims=True
        )
        h_all[t, :, j * hid : (j + 1) * hid] = (
            gate / (1.0 + jnp.exp(-gate)) * up * weight
        ).astype(jnp.bfloat16)

    def send_h(tp, device):
        send(h_all.at[tp], h_all.at[tp], h_sem.at[tp], device)

    for zz in z_list[1:]:
        send_h(t, (e, zz * CORES + c))
    send_h(t, (e, mate))
    wd_copy.wait()

    def down_part(tp, first):
        part = None
        for j in range(n_exp):
            units = pl.ds(pl.multiple_of(tp * hid, hid), hid)
            one = jnp.dot(
                h_all[tp, :, j * hid : (j + 1) * hid],
                wd_v[j, units, :],
                preferred_element_type=jnp.float32,
            )
            part = one if part is None else part + one
        if first:
            acc[...] = part
        else:
            acc[...] += part

    down_part(t, True)
    arrive(h_all.at[mate], h_sem.at[mate])
    down_part(mate, False)
    for zz in z_list[1:]:
        tp = zz * CORES + c
        arrive(h_all.at[tp], h_sem.at[tp])
        send_h(tp, (e, mate))
        down_part(tp, False)
    for zz in z_list[1:]:
        tp = zz * CORES + 1 - c
        arrive(h_all.at[tp], h_sem.at[tp])
        down_part(tp, False)

    for peer in ep_peers:
        theirs = pl.ds(pl.multiple_of(peer * rows, rows), rows)
        p_send[peer] = acc[theirs, :].astype(jnp.bfloat16)
        send(p_send.at[peer], p_recv.at[e], p_sem.at[e], (peer, t))
    combined = acc[mine, :]
    for peer in ep_peers:
        arrive(p_recv.at[peer], p_sem.at[peer])
        combined = combined + p_recv[peer].astype(jnp.float32)

    column = jnp.sum(combined * combined, axis=1, keepdims=True)
    eye = lax.broadcasted_iota(jnp.int32, (rows, LANES), 0) == lane
    s_send[...] = jnp.sum(jnp.where(eye, column, 0.0), axis=0, keepdims=True)
    for peer in tp_peers:
        send(s_send, s_all.at[t], s_sem.at[t], (e, peer))
    total = s_send[...]
    for peer in tp_peers:
        arrive(s_all.at[peer], s_sem.at[peer])
        total = total + s_all[peer]
    total = jnp.sum(jnp.where(eye, total, 0.0), axis=1, keepdims=True)
    final = lax.rsqrt(total / features + norm_eps)
    out_ref[...] = (combined * final * gain_ref[...]).astype(jnp.bfloat16)
    for copy in sends:
        copy.wait_send()


def dense_body(tokens, routing, gate_weights, w_gate, w_up, w_down, out_gain):
    n_ep, n_tp = lax.axis_size("ep"), lax.axis_size("tp")
    rows, width = tokens.shape
    n_exp, hid, features = w_gate.shape
    units, out_part = w_down.shape[1], w_down.shape[2]
    n_z = n_tp // CORES
    n_tok = rows * n_ep
    n_send = (n_z - 1) + n_ep + (n_ep - 1) + (n_z - 1) * n_ep + n_z * (n_ep - 1)
    n_send += 2 * (n_z - 1) + 1 + (n_ep - 1) + (n_tp - 1)
    vmem = pl.BlockSpec(memory_space=pltpu.VMEM)
    hbm = pl.BlockSpec(memory_space=pl.ANY)
    dma = pltpu.SemaphoreType.DMA
    return pl.pallas_call(
        functools.partial(dense_kernel, n_ep, n_tp),
        out_shape=jax.ShapeDtypeStruct((rows, out_part), jnp.bfloat16),
        in_specs=[hbm, vmem, vmem, hbm, hbm, hbm, vmem],
        out_specs=vmem,
        scratch_shapes=[
            pltpu.VMEM((n_tp, n_tok, width), jnp.bfloat16),
            pltpu.VMEM((n_tok, LANES), jnp.float32),
            pltpu.VMEM((2 * n_exp, hid, features), jnp.bfloat16),
            pltpu.VMEM((n_exp, units, out_part), jnp.bfloat16),
            pltpu.VMEM((n_tok, max(out_part, 2 * n_exp * hid)), jnp.float32),
            pltpu.VMEM((n_tp, n_tok, n_exp * hid), jnp.bfloat16),
            pltpu.VMEM((n_ep, rows, out_part), jnp.bfloat16),
            pltpu.VMEM((n_ep, rows, out_part), jnp.bfloat16),
            pltpu.VMEM((1, LANES), jnp.float32),
            pltpu.VMEM((n_tp, 1, LANES), jnp.float32),
            dma((4,)),
            dma((n_send,)),
            dma((n_ep, n_tp)),
            dma((n_ep,)),
            dma((n_tp,)),
            dma((n_ep,)),
            dma((n_tp,)),
        ],
        compiler_params=pltpu.CompilerParams(collective_id=0, has_side_effects=True),
    )(tokens, routing, gate_weights, w_gate, w_up, w_down, out_gain.reshape(1, -1))


def body(tokens, routing, gate_weights, w_gate, w_up, w_down, out_gain):
    slots = 2 * tokens.shape[0] * TOPK // (EXP_DEV * lax.axis_size("ep"))
    step = dense_body if slots >= tokens.shape[0] else routed_body
    return step(tokens, routing, gate_weights, w_gate, w_up, w_down, out_gain)


def solution(mesh):
    placed = (
        P("ep", "tp"),
        P("ep", None),
        P("ep", None),
        P("ep", "tp", None),
        P("ep", "tp", None),
        P("ep", None, "tp"),
        P("tp"),
    )
    return jax.shard_map(body, mesh=mesh, in_specs=placed, out_specs=P("ep", "tp"), check_vma=False)
```

```python
import functools

import jax
import jax.numpy as jnp
from jax import lax
from jax.experimental import pallas as pl
from jax.experimental.pallas import tpu as pltpu
from jax.sharding import PartitionSpec as P

D = 4096
TOPK = 4
EXP_DEV = 2


norm_eps = 1e-05


def routed_body(tokens, routing, gate_weights, w_gate, w_up, w_down, out_gain):
    ep_count = lax.axis_size("ep")
    tok_rows = tokens.shape[0]
    width_part = tokens.shape[1]
    experts = EXP_DEV * ep_count
    slot_count = 2 * tok_rows * TOPK // experts
    span_rows = ep_count * slot_count
    total_slots = EXP_DEV * span_rows
    flat_route = routing.reshape(-1)
    expert_ids = jnp.arange(experts, dtype=jnp.int32)
    hit_table = (flat_route[:, None] == expert_ids[None, :]).astype(jnp.int32)
    running = jnp.cumsum(hit_table, axis=0) - hit_table
    slot_rank = jnp.sum(running * hit_table, axis=1)
    slot_target = flat_route % EXP_DEV * span_rows + flat_route // EXP_DEV * slot_count + slot_rank
    entry_targets = slot_target.reshape(tok_rows, TOPK)
    slot_ids = jnp.arange(total_slots, dtype=jnp.int32)
    select_table = jnp.any(entry_targets[None, :, :] == slot_ids[:, None, None], axis=2).astype(
        jnp.bfloat16
    )
    outgoing = jnp.dot(select_table, tokens, preferred_element_type=jnp.float32).astype(
        jnp.bfloat16
    )
    outgoing = outgoing.reshape(EXP_DEV, ep_count, slot_count, width_part)
    arrived = lax.all_to_all(outgoing, "ep", split_axis=1, concat_axis=1, tiled=True).reshape(
        EXP_DEV, span_rows, width_part
    )
    piece_cols = lax.all_gather(arrived, "tp", axis=2, tiled=True)
    gate_sum = jnp.einsum("efn,esn->efs", w_gate, piece_cols, preferred_element_type=jnp.float32)
    up_sum = jnp.einsum("efn,esn->efs", w_up, piece_cols, preferred_element_type=jnp.float32)
    square_sum = jnp.einsum(
        "esn,esn->es", piece_cols, piece_cols, preferred_element_type=jnp.float32
    )
    row_scale = lax.rsqrt(square_sum / D + norm_eps)[:, None, :]
    hidden = (jax.nn.silu(gate_sum * row_scale) * (up_sum * row_scale)).astype(jnp.bfloat16)
    out_part = w_down.shape[2]
    expert_out = jnp.einsum(
        "ens,end->esd",
        lax.all_gather(hidden, "tp", axis=1, tiled=True),
        w_down,
        preferred_element_type=jnp.float32,
    ).astype(jnp.bfloat16)
    returned = lax.all_to_all(
        expert_out.reshape(EXP_DEV, ep_count, slot_count, out_part),
        "ep",
        split_axis=1,
        concat_axis=1,
        tiled=True,
    )
    returned = returned.reshape(total_slots, out_part)
    chosen = returned[slot_target].astype(jnp.float32).reshape(tok_rows, TOPK, out_part)
    combined = jnp.sum(chosen * gate_weights[:, :, None], axis=1)
    square_total = lax.psum(jnp.sum(combined * combined, axis=1), "tp")
    final_scale = lax.rsqrt(square_total / D + norm_eps)
    return (combined * final_scale[:, None] * out_gain[None, :]).astype(jnp.bfloat16)


MESH = pl.DeviceIdType.MESH
CORES = 2
LANES = 128


def dense_kernel(
    n_ep,
    n_tp,
    tok_hbm,
    route_ref,
    gates_ref,
    wg_hbm,
    wu_hbm,
    wd_hbm,
    gain_ref,
    out_ref,
    x_all,
    g_all,
    w_v,
    wd_v,
    h_all,
    p_send,
    p_recv,
    s_send,
    s_all,
    loc_sem,
    snd_sem,
    x_sem,
    g_sem,
    h_sem,
    p_sem,
    s_sem,
):
    e = lax.axis_index("ep")
    t = lax.axis_index("tp")
    n_z = n_tp // CORES
    z = t // CORES
    c = t % CORES
    mate = z * CORES + (1 - c)
    rows, width = tok_hbm.shape
    n_exp, hid = wg_hbm.shape[0], wg_hbm.shape[1]
    features = wg_hbm.shape[2]
    mine = pl.ds(pl.multiple_of(e * rows, rows), rows)

    barrier = pltpu.get_barrier_semaphore()
    tp_peers = [lax.rem(t + d, n_tp) for d in range(1, n_tp)]
    ep_list = []
    for d in range(n_ep):
        far = lax.rem(e + 2 * (d // 2), n_ep)
        ep_list.append(far + 1 - 2 * lax.rem(far, 2) if d % 2 else far)
    ep_peers = ep_list[1:]
    groups = [ep_list[:1], ep_list[1:-1], ep_list[-1:]]
    z_order = [0]
    for d in range(1, n_z // 2 + 1):
        z_order += [d] if 2 * d == n_z else [d, n_z - d]
    z_list = [lax.rem(z + d, n_z) for d in z_order]
    for peer in tp_peers:
        pl.semaphore_signal(barrier, inc=1, device_id=(e, peer), device_id_type=MESH)
    for peer in ep_peers:
        pl.semaphore_signal(barrier, inc=1, device_id=(peer, t), device_id_type=MESH)

    tok_copy = pltpu.make_async_copy(tok_hbm, x_all.at[t, mine, :], loc_sem.at[0])
    tok_copy.start()
    wg_copy = pltpu.make_async_copy(wg_hbm, w_v.at[0:n_exp], loc_sem.at[1])
    wg_copy.start()
    wu_copy = pltpu.make_async_copy(wu_hbm, w_v.at[n_exp : 2 * n_exp], loc_sem.at[2])
    wu_copy.start()
    wd_copy = pltpu.make_async_copy(wd_hbm, wd_v, loc_sem.at[3])
    wd_copy.start()

    expert = lax.broadcasted_iota(jnp.int32, (n_ep * n_exp, rows), 0)
    table = jnp.zeros((n_ep * n_exp, rows), jnp.float32)
    for k in range(route_ref.shape[0]):
        table += jnp.where(route_ref[k : k + 1, :] == expert, gates_ref[k : k + 1, :], 0.0)
    g_all[e, :, 0:rows] = table
    lane = lax.broadcasted_iota(jnp.int32, (rows, LANES), 1)
    eye = lax.broadcasted_iota(jnp.int32, (rows, LANES), 0) == lane

    sends = []

    def send(src, dst, recv, device):
        copy = pltpu.make_async_remote_copy(
            src_ref=src,
            dst_ref=dst,
            send_sem=snd_sem.at[len(sends)],
            recv_sem=recv,
            device_id=device,
            device_id_type=MESH,
        )
        copy.start()
        sends.append(copy)

    def arrive(dst, recv):
        pltpu.make_async_remote_copy(
            src_ref=dst,
            dst_ref=dst,
            send_sem=snd_sem.at[0],
            recv_sem=recv,
            device_id=(e, mate),
            device_id_type=MESH,
        ).wait_recv()

    def x_block(ep, tp):
        return x_all.at[tp, pl.ds(pl.multiple_of(ep * rows, rows), rows), :]

    def send_x(ep, tp, device):
        send(x_block(ep, tp), x_block(ep, tp), x_sem.at[ep, tp], device)

    tok_copy.wait()
    pl.semaphore_wait(barrier, n_tp - 1 + n_ep - 1)

    for zz in z_list[1:]:
        send_x(e, t, (e, zz * CORES + c))
    for peer in ep_peers:
        send_x(e, t, (peer, t))
    send_x(e, t, (e, mate))
    for peer in ep_peers:
        send(g_all.at[e], g_all.at[e], g_sem.at[e], (peer, t))
    for zz in z_list[1:]:
        tp = zz * CORES + c
        arrive(x_block(e, tp), x_sem.at[e, tp])
        for peer in ep_peers:
            send_x(e, tp, (peer, t))
        send_x(e, tp, (e, mate))
    wg_copy.wait()
    wu_copy.wait()


    def rows_of(ep):
        return pl.ds(pl.multiple_of(ep * rows, rows), rows)

    def stack(pieces):
        return pieces[0] if len(pieces) == 1 else jnp.concatenate(pieces, axis=0)

    def up_part(group, tp, state):
        x = stack([x_all[tp, rows_of(ep), :] for ep in group])
        cols = pl.ds(pl.multiple_of(tp * width, width), width)
        w = w_v[:, :, cols].reshape(2 * n_exp * hid, width)
        part = lax.dot_general(
            x, w, (((1,), (1,)), ((), ())), preferred_element_type=jnp.float32
        )
        square = jnp.zeros((x.shape[0], LANES), jnp.float32) if state is None else state[1]
        for i in range(width // LANES):
            piece = x[:, i * LANES : (i + 1) * LANES].astype(jnp.float32)
            square = square + piece * piece
        return (part if state is None else state[0] + part), square

    def h_block(ep, tp):
        return h_all.at[tp, rows_of(ep), :]

    def send_h(ep, tp, device):
        send(h_block(ep, tp), h_block(ep, tp), h_sem.at[ep, tp], device)

    def finish_hidden(group, state):
        total, square = state
        scale = lax.rsqrt(jnp.sum(square, axis=1, keepdims=True) / features + norm_eps)
        for j in range(n_exp):
            weight = stack(
                [
                    jnp.sum(
                        jnp.where(eye, g_all[ep, pl.ds(e * n_exp + j, 1), :], 0.0),
                        axis=1,
                        keepdims=True,
                    )
                    for ep in group
                ]
            )
            gate = total[:, j * hid : (j + 1) * hid] * scale
            up = total[:, (n_exp + j) * hid : (n_exp + j + 1) * hid] * scale
            part = (gate / (1.0 + jnp.exp(-gate)) * up * weight).astype(jnp.bfloat16)
            for i, ep in enumerate(group):
                h_all[t, rows_of(ep), j * hid : (j + 1) * hid] = part[i * rows : (i + 1) * rows]
        for ep in group:
            for zz in z_list[1:]:
                send_h(ep, t, (e, zz * CORES + c))
            send_h(ep, t, (e, mate))

    def relay_h(group):
        for zz in z_list[1:]:
            tp = zz * CORES + c
            for ep in group:
                arrive(h_block(ep, tp), h_sem.at[ep, tp])
                send_h(ep, tp, (e, mate))

    def down(group):
        for zz in z_list:
            tp = zz * CORES + 1 - c
            for ep in group:
                arrive(h_block(ep, tp), h_sem.at[ep, tp])
        total = None
        for tp in range(n_tp):
            h = stack([h_all[tp, rows_of(ep), :] for ep in group])
            for j in range(n_exp):
                part = jnp.dot(
                    h[:, j * hid : (j + 1) * hid],
                    wd_v[j, tp * hid : (tp + 1) * hid, :],
                    preferred_element_type=jnp.float32,
                )
                total = part if total is None else total + part
        return total

    def own_side(group, first):
        state = None
        for zz in z_list:
            tp = zz * CORES + c
            if not first:
                for ep in group:
                    arrive(x_block(ep, tp), x_sem.at[ep, tp])
                    send_x(ep, tp, (e, mate))
            state = up_part(group, tp, state)
        return state

    def mate_side(group, state):
        for zz in z_list:
            tp = zz * CORES + 1 - c
            for ep in group:
                arrive(x_block(ep, tp), x_sem.at[ep, tp])
            state = up_part(group, tp, state)
        return state

    near, middle, last = groups
    finish_hidden(near, mate_side(near, own_side(near, True)))
    for peer in ep_peers:
        arrive(g_all.at[peer], g_sem.at[peer])
    finish_hidden(middle, mate_side(middle, own_side(middle, False)))
    relay_h(near)
    finish_hidden(last, mate_side(last, own_side(last, False)))
    wd_copy.wait()
    combined = down(near)
    relay_h(middle)

    def give_back(group):
        total = down(group)
        for i, peer in enumerate(group):
            p_send[peer] = total[i * rows : (i + 1) * rows, :].astype(jnp.bfloat16)
            send(p_send.at[peer], p_recv.at[e], p_sem.at[e], (peer, t))

    give_back(middle)
    relay_h(last)
    give_back(last)
    for peer in ep_peers:
        arrive(p_recv.at[peer], p_sem.at[peer])
        combined = combined + p_recv[peer].astype(jnp.float32)

    column = jnp.sum(combined * combined, axis=1, keepdims=True)
    s_send[...] = jnp.sum(jnp.where(eye, column, 0.0), axis=0, keepdims=True)
    for peer in tp_peers:
        send(s_send, s_all.at[t], s_sem.at[t], (e, peer))
    total = s_send[...]
    for peer in tp_peers:
        arrive(s_all.at[peer], s_sem.at[peer])
        total = total + s_all[peer]
    total = jnp.sum(jnp.where(eye, total, 0.0), axis=1, keepdims=True)
    final = lax.rsqrt(total / features + norm_eps)
    out_ref[...] = (combined * final * gain_ref[...]).astype(jnp.bfloat16)
    for copy in sends:
        copy.wait_send()


def dense_body(tokens, routing, gate_weights, w_gate, w_up, w_down, out_gain):
    n_ep, n_tp = lax.axis_size("ep"), lax.axis_size("tp")
    rows, width = tokens.shape
    n_exp, hid, features = w_gate.shape
    units, out_part = w_down.shape[1], w_down.shape[2]
    n_tok = rows * n_ep
    n_send = 2 * n_ep * n_tp + 2 * n_ep + n_tp
    vmem = pl.BlockSpec(memory_space=pltpu.VMEM)
    hbm = pl.BlockSpec(memory_space=pl.ANY)
    dma = pltpu.SemaphoreType.DMA
    return pl.pallas_call(
        functools.partial(dense_kernel, n_ep, n_tp),
        out_shape=pltpu.VMEM((rows, out_part), jnp.bfloat16),
        in_specs=[hbm, vmem, vmem, hbm, hbm, hbm, vmem],
        out_specs=vmem,
        scratch_shapes=[
            pltpu.VMEM((n_tp, n_tok, width), jnp.bfloat16),
            pltpu.VMEM((n_ep, n_ep * n_exp, LANES), jnp.float32),
            pltpu.VMEM((2 * n_exp, hid, features), jnp.bfloat16),
            pltpu.VMEM((n_exp, units, out_part), jnp.bfloat16),
            pltpu.VMEM((n_tp, n_tok, n_exp * hid), jnp.bfloat16),
            pltpu.VMEM((n_ep, rows, out_part), jnp.bfloat16),
            pltpu.VMEM((n_ep, rows, out_part), jnp.bfloat16),
            pltpu.VMEM((1, LANES), jnp.float32),
            pltpu.VMEM((n_tp, 1, LANES), jnp.float32),
            dma((4,)),
            dma((n_send,)),
            dma((n_ep, n_tp)),
            dma((n_ep,)),
            dma((n_ep, n_tp)),
            dma((n_ep,)),
            dma((n_tp,)),
        ],
        compiler_params=pltpu.CompilerParams(collective_id=0, has_side_effects=True),
    )(tokens, routing.T, gate_weights.T, w_gate, w_up, w_down, out_gain.reshape(1, -1))


def body(tokens, routing, gate_weights, w_gate, w_up, w_down, out_gain):
    slots = 2 * tokens.shape[0] * TOPK // (EXP_DEV * lax.axis_size("ep"))
    step = dense_body if slots >= tokens.shape[0] else routed_body
    return step(tokens, routing, gate_weights, w_gate, w_up, w_down, out_gain)


def solution(mesh):
    placed = (
        P("ep", "tp"),
        P("ep", None),
        P("ep", None),
        P("ep", "tp", None),
        P("ep", "tp", None),
        P("ep", None, "tp"),
        P("tp"),
    )
    return jax.shard_map(body, mesh=mesh, in_specs=placed, out_specs=P("ep", "tp"), check_vma=False)
```

```python
import functools

import jax
import jax.numpy as jnp
from jax import lax
from jax.experimental import pallas as pl
from jax.experimental.pallas import tpu as pltpu
from jax.sharding import PartitionSpec as P

D = 4096
TOPK = 4
EXP_DEV = 2


norm_eps = 1e-05


def routed_body(tokens, routing, gate_weights, w_gate, w_up, w_down, out_gain):
    ep_count = lax.axis_size("ep")
    tok_rows = tokens.shape[0]
    width_part = tokens.shape[1]
    experts = EXP_DEV * ep_count
    slot_count = 2 * tok_rows * TOPK // experts
    span_rows = ep_count * slot_count
    total_slots = EXP_DEV * span_rows
    flat_route = routing.reshape(-1)
    expert_ids = jnp.arange(experts, dtype=jnp.int32)
    hit_table = (flat_route[:, None] == expert_ids[None, :]).astype(jnp.int32)
    running = jnp.cumsum(hit_table, axis=0) - hit_table
    slot_rank = jnp.sum(running * hit_table, axis=1)
    slot_target = flat_route % EXP_DEV * span_rows + flat_route // EXP_DEV * slot_count + slot_rank
    entry_targets = slot_target.reshape(tok_rows, TOPK)
    slot_ids = jnp.arange(total_slots, dtype=jnp.int32)
    select_table = jnp.any(entry_targets[None, :, :] == slot_ids[:, None, None], axis=2).astype(
        jnp.bfloat16
    )
    outgoing = jnp.dot(select_table, tokens, preferred_element_type=jnp.float32).astype(
        jnp.bfloat16
    )
    outgoing = outgoing.reshape(EXP_DEV, ep_count, slot_count, width_part)
    arrived = lax.all_to_all(outgoing, "ep", split_axis=1, concat_axis=1, tiled=True).reshape(
        EXP_DEV, span_rows, width_part
    )
    piece_cols = lax.all_gather(arrived, "tp", axis=2, tiled=True)
    gate_sum = jnp.einsum("efn,esn->efs", w_gate, piece_cols, preferred_element_type=jnp.float32)
    up_sum = jnp.einsum("efn,esn->efs", w_up, piece_cols, preferred_element_type=jnp.float32)
    square_sum = jnp.einsum(
        "esn,esn->es", piece_cols, piece_cols, preferred_element_type=jnp.float32
    )
    row_scale = lax.rsqrt(square_sum / D + norm_eps)[:, None, :]
    hidden = (jax.nn.silu(gate_sum * row_scale) * (up_sum * row_scale)).astype(jnp.bfloat16)
    out_part = w_down.shape[2]
    expert_out = jnp.einsum(
        "ens,end->esd",
        lax.all_gather(hidden, "tp", axis=1, tiled=True),
        w_down,
        preferred_element_type=jnp.float32,
    ).astype(jnp.bfloat16)
    returned = lax.all_to_all(
        expert_out.reshape(EXP_DEV, ep_count, slot_count, out_part),
        "ep",
        split_axis=1,
        concat_axis=1,
        tiled=True,
    )
    returned = returned.reshape(total_slots, out_part)
    chosen = returned[slot_target].astype(jnp.float32).reshape(tok_rows, TOPK, out_part)
    combined = jnp.sum(chosen * gate_weights[:, :, None], axis=1)
    square_total = lax.psum(jnp.sum(combined * combined, axis=1), "tp")
    final_scale = lax.rsqrt(square_total / D + norm_eps)
    return (combined * final_scale[:, None] * out_gain[None, :]).astype(jnp.bfloat16)


MESH = pl.DeviceIdType.MESH
CORES = 2
LANES = 128


def dense_kernel(
    n_ep,
    n_tp,
    tok_hbm,
    route_ref,
    gates_ref,
    wg_hbm,
    wu_hbm,
    wd_hbm,
    gain_ref,
    out_ref,
    x_all,
    g_all,
    w_v,
    wd_v,
    h_all,
    p_send,
    p_recv,
    s_send,
    s_all,
    loc_sem,
    snd_sem,
    x_sem,
    g_sem,
    h_sem,
    p_sem,
    s_sem,
):
    e = lax.axis_index("ep")
    t = lax.axis_index("tp")
    n_z = n_tp // CORES
    z = t // CORES
    c = t % CORES
    mate = z * CORES + (1 - c)
    rows, width = tok_hbm.shape
    n_exp, hid = wg_hbm.shape[0], wg_hbm.shape[1]
    features = wg_hbm.shape[2]
    mine = pl.ds(pl.multiple_of(e * rows, rows), rows)

    barrier = pltpu.get_barrier_semaphore()
    tp_peers = [lax.rem(t + d, n_tp) for d in range(1, n_tp)]
    ep_list = []
    for d in range(n_ep):
        far = lax.rem(e + 2 * (d // 2), n_ep)
        ep_list.append(far + 1 - 2 * lax.rem(far, 2) if d % 2 else far)
    ep_peers = ep_list[1:]
    groups = [ep_list[:1], ep_list[1:-1], ep_list[-1:]]
    z_order = range(n_z)
    z_list = [lax.rem(z + d, n_z) for d in z_order]
    z_give = [lax.rem(z + n_z - d, n_z) for d in z_order[1:]]
    h_list = [z] + [lax.rem(z + d, n_z) for d in z_order[1:]]
    h_give = [lax.rem(z + n_z - d, n_z) for d in z_order[1:]]
    for peer in tp_peers:
        pl.semaphore_signal(barrier, inc=1, device_id=(e, peer), device_id_type=MESH)
    for peer in ep_peers:
        pl.semaphore_signal(barrier, inc=1, device_id=(peer, t), device_id_type=MESH)

    tok_copy = pltpu.make_async_copy(tok_hbm, x_all.at[t, mine, :], loc_sem.at[0])
    tok_copy.start()
    wg_copy = pltpu.make_async_copy(wg_hbm, w_v.at[0:n_exp], loc_sem.at[1])
    wg_copy.start()
    wu_copy = pltpu.make_async_copy(wu_hbm, w_v.at[n_exp : 2 * n_exp], loc_sem.at[2])
    wu_copy.start()
    wd_copy = pltpu.make_async_copy(wd_hbm, wd_v, loc_sem.at[3])
    wd_copy.start()

    expert = lax.broadcasted_iota(jnp.int32, (n_ep * n_exp, rows), 0)
    table = jnp.zeros((n_ep * n_exp, rows), jnp.float32)
    for k in range(route_ref.shape[0]):
        table += jnp.where(route_ref[k : k + 1, :] == expert, gates_ref[k : k + 1, :], 0.0)
    g_all[e, :, 0:rows] = table
    lane = lax.broadcasted_iota(jnp.int32, (rows, LANES), 1)
    eye = lax.broadcasted_iota(jnp.int32, (rows, LANES), 0) == lane

    sends = []

    def send(src, dst, recv, device):
        copy = pltpu.make_async_remote_copy(
            src_ref=src,
            dst_ref=dst,
            send_sem=snd_sem.at[len(sends)],
            recv_sem=recv,
            device_id=device,
            device_id_type=MESH,
        )
        copy.start()
        sends.append(copy)

    def arrive(dst, recv):
        pltpu.make_async_remote_copy(
            src_ref=dst,
            dst_ref=dst,
            send_sem=snd_sem.at[0],
            recv_sem=recv,
            device_id=(e, mate),
            device_id_type=MESH,
        ).wait_recv()

    def x_block(ep, tp):
        return x_all.at[tp, pl.ds(pl.multiple_of(ep * rows, rows), rows), :]

    def send_x(ep, tp, device):
        send(x_block(ep, tp), x_block(ep, tp), x_sem.at[ep, tp], device)

    tok_copy.wait()
    pl.semaphore_wait(barrier, n_tp - 1 + n_ep - 1)

    for zz in z_give:
        send_x(e, t, (e, zz * CORES + c))
    for peer in ep_peers:
        send_x(e, t, (peer, t))
    send_x(e, t, (e, mate))
    for peer in ep_peers:
        send(g_all.at[e], g_all.at[e], g_sem.at[e], (peer, t))
    for zz in z_list[1:]:
        tp = zz * CORES + c
        arrive(x_block(e, tp), x_sem.at[e, tp])
        for peer in ep_peers:
            send_x(e, tp, (peer, t))
        send_x(e, tp, (e, mate))
    wg_copy.wait()
    wu_copy.wait()


    def rows_of(ep):
        return pl.ds(pl.multiple_of(ep * rows, rows), rows)

    def stack(pieces):
        return pieces[0] if len(pieces) == 1 else jnp.concatenate(pieces, axis=0)

    def up_part(group, tp, state):
        x = stack([x_all[tp, rows_of(ep), :] for ep in group])
        cols = pl.ds(pl.multiple_of(tp * width, width), width)
        w = w_v[:, :, cols].reshape(2 * n_exp * hid, width)
        part = lax.dot_general(
            x, w, (((1,), (1,)), ((), ())), preferred_element_type=jnp.float32
        )
        square = jnp.zeros((x.shape[0], LANES), jnp.float32) if state is None else state[1]
        for i in range(width // LANES):
            piece = x[:, i * LANES : (i + 1) * LANES].astype(jnp.float32)
            square = square + piece * piece
        return (part if state is None else state[0] + part), square

    def h_block(ep, tp):
        return h_all.at[tp, rows_of(ep), :]

    def send_h(ep, tp, device):
        send(h_block(ep, tp), h_block(ep, tp), h_sem.at[ep, tp], device)

    def finish_hidden(group, state):
        total, square = state
        scale = lax.rsqrt(jnp.sum(square, axis=1, keepdims=True) / features + norm_eps)
        for j in range(n_exp):
            weight = stack(
                [
                    jnp.sum(
                        jnp.where(eye, g_all[ep, pl.ds(e * n_exp + j, 1), :], 0.0),
                        axis=1,
                        keepdims=True,
                    )
                    for ep in group
                ]
            )
            gate = total[:, j * hid : (j + 1) * hid] * scale
            up = total[:, (n_exp + j) * hid : (n_exp + j + 1) * hid] * scale
            part = (gate / (1.0 + jnp.exp(-gate)) * up * weight).astype(jnp.bfloat16)
            for i, ep in enumerate(group):
                h_all[t, rows_of(ep), j * hid : (j + 1) * hid] = part[i * rows : (i + 1) * rows]
        for ep in group:
            for zz in h_give:
                send_h(ep, t, (e, zz * CORES + c))
            send_h(ep, t, (e, mate))

    def relay_h(group):
        for zz in h_list[1:]:
            tp = zz * CORES + c
            for ep in group:
                arrive(h_block(ep, tp), h_sem.at[ep, tp])
                send_h(ep, tp, (e, mate))

    def down(group):
        for zz in h_list:
            tp = zz * CORES + 1 - c
            for ep in group:
                arrive(h_block(ep, tp), h_sem.at[ep, tp])
        total = None
        for tp in range(n_tp):
            h = stack([h_all[tp, rows_of(ep), :] for ep in group])
            for j in range(n_exp):
                part = jnp.dot(
                    h[:, j * hid : (j + 1) * hid],
                    wd_v[j, tp * hid : (tp + 1) * hid, :],
                    preferred_element_type=jnp.float32,
                )
                total = part if total is None else total + part
        return total

    def own_side(group, first):
        state = None
        for zz in z_list:
            tp = zz * CORES + c
            if not first:
                for ep in group:
                    arrive(x_block(ep, tp), x_sem.at[ep, tp])
                    send_x(ep, tp, (e, mate))
            state = up_part(group, tp, state)
        return state

    def mate_side(group, state):
        for zz in z_list:
            tp = zz * CORES + 1 - c
            for ep in group:
                arrive(x_block(ep, tp), x_sem.at[ep, tp])
            state = up_part(group, tp, state)
        return state

    near, middle, last = groups
    finish_hidden(near, mate_side(near, own_side(near, True)))
    for peer in ep_peers:
        arrive(g_all.at[peer], g_sem.at[peer])
    finish_hidden(middle, mate_side(middle, own_side(middle, False)))
    relay_h(near)
    finish_hidden(last, mate_side(last, own_side(last, False)))
    wd_copy.wait()
    combined = down(near)
    relay_h(middle)

    def give_back(group):
        total = down(group)
        for i, peer in enumerate(group):
            p_send[peer] = total[i * rows : (i + 1) * rows, :].astype(jnp.bfloat16)
            send(p_send.at[peer], p_recv.at[e], p_sem.at[e], (peer, t))

    give_back(middle)
    relay_h(last)
    give_back(last)
    for peer in ep_peers:
        arrive(p_recv.at[peer], p_sem.at[peer])
        combined = combined + p_recv[peer].astype(jnp.float32)

    column = jnp.sum(combined * combined, axis=1, keepdims=True)
    s_send[...] = jnp.sum(jnp.where(eye, column, 0.0), axis=0, keepdims=True)
    for peer in tp_peers:
        send(s_send, s_all.at[t], s_sem.at[t], (e, peer))
    total = s_send[...]
    for peer in tp_peers:
        arrive(s_all.at[peer], s_sem.at[peer])
        total = total + s_all[peer]
    total = jnp.sum(jnp.where(eye, total, 0.0), axis=1, keepdims=True)
    final = lax.rsqrt(total / features + norm_eps)
    out_ref[...] = (combined * final * gain_ref[...]).astype(jnp.bfloat16)
    for copy in sends:
        copy.wait_send()


def dense_body(tokens, routing, gate_weights, w_gate, w_up, w_down, out_gain):
    n_ep, n_tp = lax.axis_size("ep"), lax.axis_size("tp")
    rows, width = tokens.shape
    n_exp, hid, features = w_gate.shape
    units, out_part = w_down.shape[1], w_down.shape[2]
    n_tok = rows * n_ep
    n_send = 2 * n_ep * n_tp + 2 * n_ep + n_tp
    vmem = pl.BlockSpec(memory_space=pltpu.VMEM)
    hbm = pl.BlockSpec(memory_space=pl.ANY)
    dma = pltpu.SemaphoreType.DMA
    return pl.pallas_call(
        functools.partial(dense_kernel, n_ep, n_tp),
        out_shape=pltpu.VMEM((rows, out_part), jnp.bfloat16),
        in_specs=[hbm, vmem, vmem, hbm, hbm, hbm, vmem],
        out_specs=vmem,
        scratch_shapes=[
            pltpu.VMEM((n_tp, n_tok, width), jnp.bfloat16),
            pltpu.VMEM((n_ep, n_ep * n_exp, LANES), jnp.float32),
            pltpu.VMEM((2 * n_exp, hid, features), jnp.bfloat16),
            pltpu.VMEM((n_exp, units, out_part), jnp.bfloat16),
            pltpu.VMEM((n_tp, n_tok, n_exp * hid), jnp.bfloat16),
            pltpu.VMEM((n_ep, rows, out_part), jnp.bfloat16),
            pltpu.VMEM((n_ep, rows, out_part), jnp.bfloat16),
            pltpu.VMEM((1, LANES), jnp.float32),
            pltpu.VMEM((n_tp, 1, LANES), jnp.float32),
            dma((4,)),
            dma((n_send,)),
            dma((n_ep, n_tp)),
            dma((n_ep,)),
            dma((n_ep, n_tp)),
            dma((n_ep,)),
            dma((n_tp,)),
        ],
        compiler_params=pltpu.CompilerParams(collective_id=0, has_side_effects=True),
    )(tokens, routing.T, gate_weights.T, w_gate, w_up, w_down, out_gain.reshape(1, -1))


def body(tokens, routing, gate_weights, w_gate, w_up, w_down, out_gain):
    slots = 2 * tokens.shape[0] * TOPK // (EXP_DEV * lax.axis_size("ep"))
    step = dense_body if slots >= tokens.shape[0] else routed_body
    return step(tokens, routing, gate_weights, w_gate, w_up, w_down, out_gain)


def solution(mesh):
    placed = (
        P("ep", "tp"),
        P("ep", None),
        P("ep", None),
        P("ep", "tp", None),
        P("ep", "tp", None),
        P("ep", None, "tp"),
        P("tp"),
    )
    return jax.shard_map(body, mesh=mesh, in_specs=placed, out_specs=P("ep", "tp"), check_vma=False)
```
